32 devices in a mesh: dp: 4 (over y, x), kv: 4 (over z), tp: 2 (over core).
Axes of the slice: x: 2, y: 2, z: 4, core: 2. Of those that a mesh axis runs over, the one named last changes fastest.
Arguments:
- tokens: bfloat16 [4096, 4096], P(('dp', 'kv')), parts along dimension 0, may hold values from -16 to 16
- query_weight: bfloat16 [4096, 1024], P('kv', 'tp'), may hold values from -0.09375 to 0.09375
- key_weight: bfloat16 [4096, 256], P('kv', 'tp'), may hold values from -0.09375 to 0.09375
- value_weight: bfloat16 [4096, 256], P('kv', 'tp'), may hold values from -0.09375 to 0.09375
- out_weight: bfloat16 [1024, 4096], P('kv', 'tp'), may hold values from -1.5 to 1.5
- chosen: int32 [128, 16], P(('dp', 'kv')), parts along dimension 0, may hold values from -1 to 31, as said below
- live_length: int32 [4], P('dp'), parts along dimension 0, may hold values from 128 to 1024
Outputs:
- mixed: bfloat16 [4096, 4096], P(('dp', 'kv'), 'tp'), parts along dimension 0
The draws below stay inside these ranges and needn't reach their ends.
There are 4 independent parts, one for each index of `dp`. The reference program is written for one: setup_inputs(seed, part) draws one part's arguments, and reference() takes and returns one part's arrays. A program takes and returns all parts, laid end to end along the dimension named above; an argument that names none is the same for every part. Nothing has to cross between parts.
Inputs may be any that keep to these rules, and one draw needn't show every extreme that they name: `chosen`: row j lists 16 entries: entry 0 is j itself, the others are distinct blocks before j, or -1 for unused entries. The query blocks of one device together read at most 2 distinct blocks held by any one other device, and some device reads 2 of another's in every draw.
All inputs are finite; a program needn't handle non-finite values.
Results may differ from the reference program's by a relative error of at most 0.0085.
Values may be sent and summed in bfloat16 or wider, within the bound.
A program may use at most 64 MiB of HBM per device.

```python
import jax
import jax.numpy as jnp
from jax import lax

D = 4096
HEADS = 8
KV_HEADS = 2
HD = 128
BLOCK = 32
NSEL = 16
CAP = 2
TOK_DEV = 256
TOKENS = 1024
SEGMENT_TOTAL = 32
Q_WIDTH = 1024
KV_WIDTH = 256
N_KV = 4


def draw_tokens(key, part):
    normal_draw = jax.random.normal(key, (TOKENS, D), jnp.float32)
    return jnp.clip(normal_draw, -6.0, 6.0).astype(jnp.bfloat16)


def draw_chosen(key, part):
    owners = TOKENS // TOK_DEV
    per_dev = TOK_DEV // BLOCK
    pick_key = jax.random.fold_in(key, 11)
    noise_key = jax.random.fold_in(key, 13)
    pick_scores = jax.random.randint(pick_key, (owners, owners, per_dev), 0, 1 << 20)
    local_ids = jnp.arange(per_dev, dtype=jnp.int32)
    order = jnp.argsort(pick_scores * per_dev + local_ids[None, None, :], axis=-1, stable=True)
    allowed_local = order[..., :CAP]
    allowed = jnp.any(local_ids[None, None, None, :] == allowed_local[..., None], axis=2)
    allowed = allowed.reshape(owners, SEGMENT_TOTAL)
    stream_segments = jnp.arange(SEGMENT_TOTAL, dtype=jnp.int32)
    segment_loader = stream_segments // per_dev
    segment_retainer = stream_segments // per_dev
    remote_segment = allowed[segment_loader] & (segment_retainer[None, :] < segment_loader[:, None])
    local = (segment_retainer[None, :] == segment_loader[:, None]) & (stream_segments[None, :] < stream_segments[:, None])
    eligible_filter = remote_segment | local
    rating_increment = jnp.where(remote_segment & (segment_retainer[None, :] == 0), 2, jnp.where(remote_segment & (segment_retainer[None, :] == segment_loader[:, None] - 1), 1, 0))
    stochastic_perturbation = jax.random.randint(noise_key, (SEGMENT_TOTAL, SEGMENT_TOTAL), 0, 1 << 12)
    segment_rating = jnp.where(eligible_filter, (stochastic_perturbation + rating_increment * (1 << 12)) * SEGMENT_TOTAL + stream_segments[None, :], -1)
    values, indices = lax.top_k(segment_rating, NSEL - 1)
    picks = jnp.where(values >= 0, indices, -1).astype(jnp.int32)
    return jnp.concatenate([stream_segments[:, None], picks], axis=1).astype(jnp.int32)


def level_of(rng, shape, split, least, high):
    def one(axis_at, parts):
        draws = jax.random.uniform(jax.random.fold_in(jax.random.fold_in(rng, 6), axis_at), (parts,), jnp.float32, least / len(split), high / len(split))
        return jnp.repeat(jnp.exp(draws), shape[axis_at] // parts).reshape((-1,) + (1,) * (len(shape) - axis_at - 1))

    loudness = one(*split[0])
    for cut in split[1:]:
        loudness = loudness * one(*cut)
    return loudness


def scatter_about(key, extent, width, bound, split=(), held_as=jnp.bfloat16):
    values = jax.random.normal(key, extent, jnp.float32) * width
    if len(split) > 0:
        values = level_of(key, extent, split, -0.22, 0.18) * values
    return jnp.clip(values, min=-bound, max=bound).astype(held_as)


def setup_inputs(seed: int = 0, part: int = 0) -> dict:
    key_list = jax.random.split(jax.random.key(seed), 8)
    part_splits = jax.random.split(jax.random.fold_in(key_list[7], part), 8)
    return {
        "tokens": draw_tokens(jax.random.fold_in(jax.random.fold_in(key_list[7], part), 71), part),
        "query_weight": scatter_about(key_list[1], (D, Q_WIDTH), D ** -0.5, 0.09375, ((0, 4), (1, 2))),
        "key_weight": scatter_about(key_list[2], (D, KV_WIDTH), D ** -0.5, 0.09375, ((0, 4), (1, 2))),
        "value_weight": scatter_about(key_list[3], (D, KV_WIDTH), D ** -0.5, 0.09375, ((0, 4), (1, 2))),
        "out_weight": scatter_about(key_list[4], (Q_WIDTH, D), (Q_WIDTH // 64) ** -0.5, 1.5, ((0, 4), (1, 2))),
        "chosen": draw_chosen(jax.random.fold_in(jax.random.fold_in(key_list[7], part), 71), part),
        "live_length": jax.random.randint(part_splits[6], (1,), TOKENS // 8, TOKENS + 1).astype(jnp.int32),
    }


def reference(tokens, query_weight, key_weight, value_weight, out_weight, chosen, live_length):
    queries = jnp.dot(tokens, query_weight, preferred_element_type=jnp.float32).astype(jnp.bfloat16)
    keys = jnp.dot(tokens, key_weight, preferred_element_type=jnp.float32).astype(jnp.bfloat16)
    values = jnp.dot(tokens, value_weight, preferred_element_type=jnp.float32).astype(jnp.bfloat16)
    groups = HEADS // KV_HEADS
    per_dev = TOK_DEV // BLOCK
    key_blocks = keys.reshape(SEGMENT_TOTAL, BLOCK, KV_HEADS, HD)
    value_blocks = values.reshape(SEGMENT_TOTAL, BLOCK, KV_HEADS, HD)
    query_parts = queries.reshape(N_KV, per_dev, BLOCK, KV_HEADS, groups, HD)
    chosen_parts = chosen.reshape(N_KV, per_dev, NSEL)
    firsts = (jnp.arange(N_KV) * per_dev).astype(jnp.int32)
    limit = live_length[0]

    def attend(item):
        q_part, picks, first = item
        valid = picks >= 0
        safe = jnp.maximum(picks, 0)
        near_keys = key_blocks[safe].astype(jnp.float32)
        near_values = value_blocks[safe].astype(jnp.float32)
        scores = jnp.einsum("jqkgd,jnbkd->jkgqnb", q_part.astype(jnp.float32), near_keys) * (HD ** -0.5)
        query_pos = (first + jnp.arange(per_dev, dtype=jnp.int32))[:, None] * BLOCK + jnp.arange(BLOCK, dtype=jnp.int32)[None, :]
        key_pos = safe[:, :, None] * BLOCK + jnp.arange(BLOCK, dtype=jnp.int32)[None, None, :]
        allowed = valid[:, None, :, None] & (key_pos[:, None, :, :] <= query_pos[:, :, None, None])
        masked = jnp.where(allowed[:, None, None], scores, -jnp.inf)
        top = jnp.max(masked, axis=(4, 5), keepdims=True)
        weights = jnp.exp(masked - top)
        total = jnp.sum(weights, axis=(4, 5))
        rounded = lax.optimization_barrier(weights.astype(jnp.bfloat16)).astype(jnp.float32)
        summed = jnp.einsum("jkgqnb,jnbkd->jqkgd", rounded, near_values)
        result = summed / jnp.transpose(total, (0, 3, 1, 2))[..., None]
        live = query_pos < limit
        result = jnp.where(live[:, :, None, None, None], result, 0.0)
        return result.astype(jnp.bfloat16)

    attended = lax.map(attend, (query_parts, chosen_parts, firsts)).reshape(TOKENS, Q_WIDTH)
    return jnp.dot(attended, out_weight, preferred_element_type=jnp.float32).astype(jnp.bfloat16)
```

```python
import functools

import jax
import jax.numpy as jnp
from jax import lax
from jax.experimental import pallas as pl
from jax.experimental.pallas import tpu as pltpu
from jax.sharding import PartitionSpec as P

HD = 128
BLOCK = 32
CAP = 2
MESH = pl.DeviceIdType.MESH


def gathered_body(tokens, query_weight, key_weight, value_weight, out_weight, chosen, live_length):
    rows = tokens.shape[0]
    per_dev = rows // BLOCK
    owners = lax.axis_size("kv")
    me = lax.axis_index("kv")

    def add_rows(piece):
        return jnp.dot(tokens, piece, preferred_element_type=jnp.float32)

    queries = add_rows(lax.all_gather(query_weight, "kv", axis=0, tiled=True))
    keys = add_rows(lax.all_gather(key_weight, "kv", axis=0, tiled=True))
    values = add_rows(lax.all_gather(value_weight, "kv", axis=0, tiled=True))
    queries = queries.astype(jnp.bfloat16)
    paired = jnp.concatenate([keys.astype(jnp.bfloat16), values.astype(jnp.bfloat16)], axis=1)
    width = paired.shape[1]
    local_blocks = paired.reshape(per_dev, BLOCK, width)
    valid = chosen >= 0
    safe = jnp.maximum(chosen, 0)
    blocks_all = owners * per_dev
    hits = (safe[:, :, None] == jnp.arange(blocks_all, dtype=jnp.int32)[None, None, :]) & valid[
        :, :, None
    ]
    needed = jnp.any(hits, axis=(0, 1)).reshape(owners, per_dev)
    needed = needed & (jnp.arange(owners, dtype=jnp.int32) != me)[:, None]
    ranks = jnp.cumsum(needed.astype(jnp.int32), axis=1)
    local_ids = jnp.arange(per_dev, dtype=jnp.int32)
    slot_lists = []
    for slot in range(CAP):
        marked = needed & (ranks == slot + 1)
        found = jnp.any(marked, axis=1)
        where_at = jnp.sum(jnp.where(marked, local_ids[None, :], 0), axis=1)
        slot_lists.append(jnp.where(found, where_at, -1))
    wanted = jnp.stack(slot_lists, axis=1)
    requested = lax.all_to_all(wanted, "kv", split_axis=0, concat_axis=0, tiled=True)
    outgoing = local_blocks[jnp.maximum(requested, 0)]
    outgoing = jnp.where((requested >= 0)[:, :, None, None], outgoing, jnp.zeros((), jnp.bfloat16))
    incoming = lax.all_to_all(outgoing, "kv", split_axis=0, concat_axis=0, tiled=True)
    table = jnp.concatenate([incoming.reshape(owners * CAP, BLOCK, width), local_blocks], axis=0)
    segment_retainer = safe // per_dev
    local_of = safe % per_dev
    match = (wanted[None, None, :, :] == local_of[:, :, None, None]) & (
        jnp.arange(owners, dtype=jnp.int32)[None, None, :, None]
        == segment_retainer[:, :, None, None]
    )
    slot_index = jnp.arange(owners * CAP, dtype=jnp.int32).reshape(owners, CAP)
    remote_at = jnp.sum(jnp.where(match, slot_index[None, None], 0), axis=(2, 3))
    position = jnp.where(segment_retainer == me, owners * CAP + local_of, remote_at)
    picked = table[position]
    near_keys = picked[..., :HD]
    near_values = picked[..., HD:]
    grouped = queries.reshape(per_dev, BLOCK, -1, HD)
    scores = jnp.einsum(
        "jqhd,jnbd->jhqnb", grouped, near_keys, preferred_element_type=jnp.float32
    ) * HD ** (-0.5)
    query_pos = (me * per_dev + jnp.arange(per_dev, dtype=jnp.int32))[:, None] * BLOCK + jnp.arange(
        BLOCK, dtype=jnp.int32
    )[None, :]
    key_pos = safe[:, :, None] * BLOCK + jnp.arange(BLOCK, dtype=jnp.int32)[None, None, :]
    allowed = valid[:, None, :, None] & (key_pos[:, None, :, :] <= query_pos[:, :, None, None])
    masked = jnp.where(allowed[:, None], scores, -jnp.inf)
    top = jnp.max(masked, axis=(3, 4), keepdims=True)
    weights = jnp.exp(masked - top)
    total = jnp.sum(weights, axis=(3, 4))
    summed = jnp.einsum(
        "jhqnb,jnbd->jqhd",
        weights.astype(jnp.bfloat16),
        near_values,
        preferred_element_type=jnp.float32,
    )
    result = summed / jnp.transpose(total, (0, 2, 1))[..., None]
    live = query_pos < live_length[0]
    result = jnp.where(live[:, :, None, None], result, 0.0)
    attended = result.astype(jnp.bfloat16).reshape(rows, -1)
    every_head = lax.all_gather(attended, "tp", axis=1, tiled=True)
    mixed = jnp.dot(
        every_head,
        lax.all_gather(out_weight, "kv", axis=0, tiled=True),
        preferred_element_type=jnp.float32,
    )
    return mixed.astype(jnp.bfloat16)


class Stream:
    def __init__(self, place, full, first, rows, halved, sends, recvs, base):
        self.place, self.full, self.halved = place, full, halved
        self.shard = full.shape[0] // place["n"]
        self.first, self.rows = first, rows
        self.sends, self.recvs, self.base = sends, recvs, base
        self.begun = []

    def part(self, owner, index, count):
        size = self.rows // count
        start = pl.multiple_of(owner * self.shard + self.first + index * size, size)
        return self.full.at[pl.ds(start, size), :]

    def carried(self, owner):
        if self.halved:
            return self.part(owner, self.place["half"], 2)
        return self.part(owner, self.place["dp"], 4)

    def copy(self, part, owner, kind, target, sent_as=None):
        at = self.base + owner * 5
        return pltpu.make_async_remote_copy(
            src_ref=part,
            dst_ref=part,
            send_sem=self.sends.at[at + (kind if sent_as is None else sent_as)],
            recv_sem=self.recvs.at[at + kind],
            device_id=target,
            device_id_type=MESH,
        )

    def begin(self, c, when=None):
        if when is None:
            c.start()
        else:
            pl.when(when)(c.start)
        self.begun.append((c, when))

    def issue(self):
        p = self.place
        me, n = p["me"], p["n"]
        mine = self.carried(me)
        self.begin(self.copy(mine, me, 0, {"kv": p["right"]}), me < n - 1)
        self.begin(self.copy(mine, me, 0, {"kv": p["left"]}, 1), me > 0)

    def relay(self, slot):
        p = self.place
        me, n, owner = p["me"], p["n"], p["order"][slot]
        piece = self.carried(owner)
        self.copy(piece, owner, 0, {"kv": p["right"]}).wait_recv()
        self.begin(
            self.copy(piece, owner, 0, {"kv": p["right"]}), jnp.logical_and(owner < me, me < n - 1)
        )
        self.begin(self.copy(piece, owner, 0, {"kv": p["left"]}, 0), jnp.logical_and(owner > me, me > 0))
        if self.halved:
            to_x = self.part(owner, 2 * p["half"], 4)
            to_y = self.part(owner, 2 * p["half"] + 1, 4)
        else:
            to_x = to_y = piece
        self.begin(self.copy(to_x, owner, 1, {"dp": p["x"]}))
        self.begin(self.copy(to_y, owner, 2, {"dp": p["y"]}))

    def corner(self, slot):
        p = self.place
        owner = p["order"][slot]
        if self.halved:
            other = 2 * (1 - p["half"])
            self.copy(self.part(owner, other, 4), owner, 1, {"dp": p["x"]}).wait_recv()
            self.copy(self.part(owner, other + 1, 4), owner, 2, {"dp": p["y"]}).wait_recv()
            return
        self.copy(self.part(owner, p["x"], 4), owner, 1, {"dp": p["x"]}).wait_recv()
        self.begin(self.copy(self.part(owner, 2 * p["x"], 8), owner, 4, {"dp": p["y"]}))
        self.copy(self.part(owner, p["y"], 4), owner, 2, {"dp": p["y"]}).wait_recv()
        self.begin(self.copy(self.part(owner, 2 * p["y"] + 1, 8), owner, 3, {"dp": p["x"]}))

    def arrive(self):
        p = self.place
        if self.halved:
            return
        for owner in p["order"]:
            self.copy(self.part(owner, 2 * p["far"], 8), owner, 4, {"dp": p["y"]}).wait_recv()
            self.copy(self.part(owner, 2 * p["far"] + 1, 8), owner, 3, {"dp": p["x"]}).wait_recv()

    def finish(self):
        for c, when in self.begun:
            if when is None:
                c.wait_send()
            else:
                pl.when(when)(c.wait_send)


def kernel(
    n, chosen, live, tokens, query_w, key_w, value_w, out_w, mixed,
    tok, full_q, full_k, full_v, full_o, paired, queries, bias, attended,
    local_sem, send_sem, recv_sem, kv_send, kv_recv, tp_send, tp_recv,
):
    dp, me, tp = lax.axis_index("dp"), lax.axis_index("kv"), lax.axis_index("tp")
    x_at, y_at = lax.rem(dp, 2), lax.div(dp, 2)
    place = {
        "n": n,
        "me": me,
        "left": lax.rem(me + n - 1, n),
        "right": lax.rem(me + 1, n),
        "opp": lax.rem(me + 2, n),
        "x": 2 * y_at + (1 - x_at),
        "y": 2 * (1 - y_at) + x_at,
        "half": lax.rem(x_at + y_at, 2),
        "dp": dp,
        "far": 2 * (1 - y_at) + (1 - x_at),
    }
    order = []
    for i in range(n - 1):
        up = i + (i >= me).astype(jnp.int32)
        down = n - 1 - i - (n - 1 - i <= me).astype(jnp.int32)
        order.append(jnp.where(2 * me < n, up, down))
    place["order"] = order
    rows = tok.shape[0]
    per_dev = rows // BLOCK
    seq = n * rows

    fulls = (full_k, full_v, full_q, full_o)
    loads = []
    for index, (shard, full) in enumerate(zip((key_w, value_w, query_w, out_w), fulls)):
        size = shard.shape[0]
        mine = full.at[pl.ds(pl.multiple_of(me * size, size), size), :]
        loads.append(pltpu.make_async_copy(shard, mine, local_sem.at[index]))
    loads.append(pltpu.make_async_copy(tokens, tok, local_sem.at[4]))
    for load in loads:
        load.start()

    barrier = pltpu.get_barrier_semaphore()
    greeted = [{"kv": place[k]} for k in ("left", "right", "opp")]
    greeted += [{"dp": place[k]} for k in ("x", "y")] + [{"tp": 1 - tp}]
    for target in greeted:
        pl.semaphore_signal(barrier, inc=1, device_id=target, device_id_type=MESH)
    pl.semaphore_wait(barrier, len(greeted))

    cut = full_o.shape[0] // n // 2
    plan = [(full_k, 0, 0), (full_v, 0, 0), (full_q, 0, 0), (full_o, 0, 0), (full_o, cut, 1)]
    streams = []
    for i, (full, first, halved) in enumerate(plan):
        count = cut if full is full_o else full.shape[0] // n
        streams.append(
            Stream(place, full, first, count, halved, send_sem, recv_sem, 5 * n * i)
        )
    groups = [streams[:2], streams[2:3], streams[3:4], streams[4:5]]
    each = n - 1

    def advance(at):
        group, slot = divmod(at, each)
        if group < len(groups):
            for s in groups[group]:
                s.relay(slot)
            if slot == 0 and group + 1 < len(groups):
                for s in groups[group + 1]:
                    s.issue()
        if at > 0:
            group, slot = divmod(at - 1, each)
            for s in groups[group]:
                s.corner(slot)

    loads[0].wait()
    loads[1].wait()
    for s in groups[0]:
        s.issue()
    loads[2].wait()
    loads[3].wait()
    loads[4].wait()

    column = lax.broadcasted_iota(jnp.int32, (BLOCK, seq), 1)
    row = lax.broadcasted_iota(jnp.int32, (BLOCK, seq), 0)
    key_block = lax.div(lax.broadcasted_iota(jnp.int32, (8, seq), 1), BLOCK)
    for j in range(per_dev):
        listed = jnp.full((8, seq), -jnp.inf, jnp.float32)
        for e in range(chosen.shape[1]):
            listed = jnp.where(key_block == chosen[j, e], 0.0, listed)
        spread = jnp.concatenate([listed] * (BLOCK // 8), axis=0)
        causal = column <= row + (me * rows + j * BLOCK)
        bias[j * BLOCK : (j + 1) * BLOCK, :] = jnp.where(causal, spread, -jnp.inf)

    for at in range(each + 2):
        advance(at)
    for s in groups[0]:
        s.arrive()
    mine = pl.ds(pl.multiple_of(me * rows, rows), rows)
    paired[mine, :HD] = jnp.dot(
        tok[...], full_k[...], preferred_element_type=jnp.float32
    ).astype(jnp.bfloat16)
    paired[mine, HD:] = jnp.dot(
        tok[...], full_v[...], preferred_element_type=jnp.float32
    ).astype(jnp.bfloat16)
    advance(each + 2)
    kv_copies = []
    for step in range(1, n):
        block = paired.at[mine, :]
        c = pltpu.make_async_remote_copy(
            src_ref=block, dst_ref=block,
            send_sem=kv_send.at[step - 1], recv_sem=kv_recv.at[step - 1],
            device_id={"kv": lax.rem(me + step, n)}, device_id_type=MESH,
        )
        c.start()
        kv_copies.append(c)
    for at in range(each + 3, 2 * each + 2):
        advance(at)
    groups[1][0].arrive()
    queries[...] = jnp.dot(
        tok[...], full_q[...], preferred_element_type=jnp.float32
    ).astype(jnp.bfloat16)
    advance(2 * each + 2)
    for step in range(1, n):
        owner = lax.rem(me + n - step, n)
        block = paired.at[pl.ds(pl.multiple_of(owner * rows, rows), rows), :]
        pltpu.make_async_remote_copy(
            src_ref=block, dst_ref=block,
            send_sem=kv_send.at[step - 1], recv_sem=kv_recv.at[step - 1],
            device_id={"kv": lax.rem(me + step, n)}, device_id_type=MESH,
        ).wait_recv()

    position = me * rows + lax.broadcasted_iota(jnp.int32, (rows, HD), 0)
    alive = position < live[0]
    heads = queries.shape[1] // HD
    for h in range(heads):
        cols = slice(h * HD, (h + 1) * HD)
        scores = lax.dot_general(
            queries[:, cols], paired[:, :HD], (((1,), (1,)), ((), ())),
            preferred_element_type=jnp.float32,
        )
        masked = scores * HD ** (-0.5) + bias[...]
        top = jnp.max(masked, axis=1, keepdims=True)
        weights = jnp.exp(masked - top)
        total = jnp.sum(weights, axis=1, keepdims=True)
        summed = jnp.dot(
            weights.astype(jnp.bfloat16), paired[:, HD:], preferred_element_type=jnp.float32
        )
        result = jnp.where(alive, summed / total, 0.0).astype(jnp.bfloat16)
        attended[tp, :, cols] = result
        if h == heads // 2 - 1:
            advance(2 * each + 3)
    share = pltpu.make_async_remote_copy(
        src_ref=attended.at[tp], dst_ref=attended.at[tp],
        send_sem=tp_send, recv_sem=tp_recv, device_id={"tp": 1 - tp}, device_id_type=MESH,
    )
    share.start()
    for at in range(2 * each + 4, len(groups) * each + 1):
        advance(at)
    pltpu.make_async_remote_copy(
        src_ref=attended.at[1 - tp], dst_ref=attended.at[1 - tp],
        send_sem=tp_send, recv_sem=tp_recv, device_id={"tp": 1 - tp}, device_id_type=MESH,
    ).wait_recv()
    for s in groups[2] + groups[3]:
        s.arrive()
    wide = queries.shape[1]
    tile = 512
    for c in range(0, mixed.shape[1], tile):
        acc = jnp.dot(
            attended[0], full_o[:wide, c : c + tile], preferred_element_type=jnp.float32
        )
        acc += jnp.dot(
            attended[1], full_o[wide:, c : c + tile], preferred_element_type=jnp.float32
        )
        mixed[:, c : c + tile] = acc.astype(jnp.bfloat16)
    for s in streams:
        s.finish()
    for c in kv_copies:
        c.wait_send()
    share.wait_send()


def woven_body(tokens, query_weight, key_weight, value_weight, out_weight, chosen, live_length):
    n = lax.axis_size("kv")
    rows, width = tokens.shape
    wide = query_weight.shape[1]
    dma = pltpu.SemaphoreType.DMA
    bf16 = jnp.bfloat16
    anywhere = pl.BlockSpec(memory_space=pl.ANY)
    small = pl.BlockSpec(memory_space=pltpu.SMEM)
    return pl.pallas_call(
        functools.partial(kernel, n),
        out_shape=jax.ShapeDtypeStruct((rows, out_weight.shape[1]), bf16),
        in_specs=[small, small] + [anywhere] * 5,
        out_specs=pl.BlockSpec(memory_space=pltpu.VMEM),
        scratch_shapes=[
            pltpu.VMEM((rows, width), bf16),
            pltpu.VMEM((width, wide), bf16),
            pltpu.VMEM((width, HD), bf16),
            pltpu.VMEM((width, HD), bf16),
            pltpu.VMEM((n * out_weight.shape[0], out_weight.shape[1]), bf16),
            pltpu.VMEM((n * rows, 2 * HD), bf16),
            pltpu.VMEM((rows, wide), bf16),
            pltpu.VMEM((rows, n * rows), jnp.float32),
            pltpu.VMEM((2, rows, wide), bf16),
            dma((5,)),
            dma((5 * 5 * n,)),
            dma((5 * 5 * n,)),
            dma((n - 1,)),
            dma((n - 1,)),
            dma,
            dma,
        ],
        compiler_params=pltpu.CompilerParams(
            collective_id=0, has_side_effects=True, vmem_limit_bytes=56 * 2**20
        ),
    )(chosen, live_length, tokens, query_weight, key_weight, value_weight, out_weight)


def solution(mesh):
    in_specs = (
        P(("dp", "kv"), None),
        P("kv", "tp"),
        P("kv", "tp"),
        P("kv", "tp"),
        P("kv", "tp"),
        P(("dp", "kv"), None),
        P("dp"),
    )
    out_specs = P(("dp", "kv"), "tp")
    fits = (mesh.shape["dp"], mesh.shape["kv"], mesh.shape["tp"]) == (4, 4, 2)
    body = woven_body if fits else gathered_body
    return jax.shard_map(body, mesh=mesh, in_specs=in_specs, out_specs=out_specs, check_vma=False)
```
